32 devices in a mesh: grp: 2 (over y), kv: 4 (over z), tp: 4 (over x, core).
Axes of the slice: x: 2, y: 2, z: 4, core: 2. Of those that a mesh axis runs over, the one named last changes fastest.
Arguments:
- tokens: bfloat16 [128, 2048], P('grp', 'kv'), parts along dimension 0, may hold values from -64 to 64
- lengths: int32 [128], P(('grp', 'kv')), parts along dimension 0, may hold values from 1 to 4096, 32768 in all
- state: float32 [128, 8, 128, 256], P(('grp', 'kv'), 'tp'), parts along dimension 0, may hold values from -6 to 6
- key_block: bfloat16 [128, 8, 64, 128], P(('grp', 'kv'), 'tp'), parts along dimension 0, may hold values from -6 to 6
- value_block: bfloat16 [128, 8, 64, 256], P(('grp', 'kv'), 'tp'), parts along dimension 0, may hold values from -6 to 6
- cum_decay: float32 [128, 8, 64, 128], P(('grp', 'kv'), 'tp'), parts along dimension 0, as said below
- step_decay: float32 [128, 1024], P(('grp', 'kv'), 'tp'), parts along dimension 0
- g_mix: bfloat16 [2048], P('kv'), may hold values from 0.099609375 to 1.8984375
- w_query: bfloat16 [2048, 1024], P('kv', 'tp'), may hold values from -0.125 to 0.125
- w_key: bfloat16 [2048, 1024], P('kv', 'tp'), may hold values from -0.125 to 0.125
- w_value: bfloat16 [2048, 2048], P('kv', 'tp'), may hold values from -0.125 to 0.125
- w_outgate: bfloat16 [2048, 2048], P('kv', 'tp'), may hold values from -0.125 to 0.125
- w_decay: bfloat16 [2048, 1024], P('kv', 'tp'), may hold values from -0.5 to 0.5
- g_heads: bfloat16 [2048], P('tp'), may hold values from 0.099609375 to 1.8984375
- w_out: bfloat16 [2048, 2048], P('tp', 'kv'), may hold values from -0.125 to 0.125
- g_ffn: bfloat16 [2048], P('kv'), may hold values from 0.099609375 to 1.8984375
- w_gate: bfloat16 [2048, 5632], P('kv', 'tp'), may hold values from -0.125 to 0.125
- w_up: bfloat16 [2048, 5632], P('kv', 'tp'), may hold values from -0.125 to 0.125
- w_down: bfloat16 [5632, 2048], P('tp', 'kv'), may hold values from -0.078125 to 0.078125
Outputs:
- updated: bfloat16 [128, 2048], P('grp', 'kv'), parts along dimension 0
The draws below stay inside these ranges and needn't reach their ends.
There are 2 independent parts, one for each index of `grp`. The reference program is written for one: setup_inputs(seed, part) draws one part's arguments, and reference() takes and returns one part's arrays. A program takes and returns all parts, laid end to end along the dimension named above; an argument that names none is the same for every part. Nothing has to cross between parts.
Inputs may be any that keep to these rules, and one draw needn't show every extreme that they name: `cum_decay`: along the block's positions the entries never rise.
All inputs are finite; a program needn't handle non-finite values. No bound on the sum of `lengths` on one device may be relied on, other than what follows from the above.
Results may differ from the reference program's by a relative error of at most 0.019.
Values may be sent and summed in bfloat16 or wider, within the bound.
No kernel may reach another device: no remote copies, remote signals or barrier semaphores. Data moves between devices by JAX's collectives and lax.ppermute only.
A program may use at most 64 MiB of HBM per device.

```python
import math
import jax
import jax.numpy as jnp
import numpy as np
from jax import lax

D = 2048
ATTN_GROUPS = 8
DK = 128
DV = 256
FF = 5632
SPAN_STEPS = 64
STREAM_NUMBER = 64
N_TP = 4


def head_rates(key):
    k_slow, k_fast, k_seq, k_chan = jax.random.split(key, 4)
    gradual_shrink_factor = jax.random.bernoulli(k_slow, 0.5, (1, ATTN_GROUPS, 1))
    fast_rate = jax.random.uniform(k_fast, (1, ATTN_GROUPS, 1), jnp.float32, 1.0 / 50.0, 1.0 / 30.0)
    slow_rate = jnp.float32(0.5 / SPAN_STEPS)
    seq_factor = jnp.exp(jax.random.uniform(k_seq, (STREAM_NUMBER, 1, 1), jnp.float32, math.log(0.5), math.log(2.0)))
    chan_factor = jax.random.uniform(k_chan, (1, ATTN_GROUPS, DK), jnp.float32, 0.5, 1.5)
    rate = jnp.where(gradual_shrink_factor, slow_rate, fast_rate) * seq_factor * chan_factor
    return (rate, gradual_shrink_factor)


def draw_tokens(key, part):
    k_base, k_rise, k_rows = jax.random.split(key, 3)
    columns = jnp.arange(D, dtype=jnp.float32) / D
    rough = jax.random.uniform(k_rise, (D,), jnp.float32, 0.5, 2.0)
    rows = jnp.exp(jax.random.uniform(k_rows, (STREAM_NUMBER, 1), jnp.float32, math.log(0.3), math.log(3.0)))
    base = jnp.clip(jax.random.normal(k_base, (STREAM_NUMBER, D), jnp.float32), -6.0, 6.0)
    rise = 3.0 ** columns * rough / 1.8
    return (base * rise[None, :] * rows).astype(jnp.bfloat16)


def draw_cum_decay(key, part):
    rate, gradual_shrink_factor = head_rates(jax.random.fold_in(key, 11))
    k_step, lookup_location, lookup_breadth = jax.random.split(jax.random.fold_in(key, 12), 3)
    steps = -rate[:, :, None, :] * jax.random.uniform(k_step, (STREAM_NUMBER, ATTN_GROUPS, SPAN_STEPS, DK), jnp.float32, 0.5, 1.5)
    span_offset = jax.random.randint(lookup_location, (STREAM_NUMBER, ATTN_GROUPS, 1, 2), 0, SPAN_STEPS)
    token_ordinal = jnp.arange(SPAN_STEPS, dtype=jnp.int32)[None, None, :, None]
    match_tally = jnp.any(token_ordinal == span_offset, axis=3)
    span_extent = jnp.log(jax.random.uniform(lookup_breadth, (STREAM_NUMBER, ATTN_GROUPS, 1), jnp.float32, 0.5, 0.8))
    surplus_tally = jnp.where(match_tally & gradual_shrink_factor, span_extent, jnp.float32(0.0))
    steps = steps + surplus_tally[:, :, :, None]
    return jnp.cumsum(steps, axis=2).astype(jnp.float32)


def draw_step_decay(key, part):
    rate, gradual_shrink_factor = head_rates(jax.random.fold_in(key, 11))
    k_step, lookup_location, lookup_breadth = jax.random.split(jax.random.fold_in(key, 13), 3)
    k_rough = jax.random.fold_in(key, 14)
    payload_element = -rate * jax.random.uniform(k_step, (STREAM_NUMBER, ATTN_GROUPS, DK), jnp.float32, 0.5, 1.5)
    payload_element = payload_element - jax.random.uniform(k_rough, (STREAM_NUMBER, ATTN_GROUPS, DK), jnp.float32, 0.0, 0.35)
    match_tally = jax.random.randint(lookup_location, (STREAM_NUMBER, ATTN_GROUPS, 1), 0, 2) == 0
    span_extent = jnp.log(jax.random.uniform(lookup_breadth, (STREAM_NUMBER, ATTN_GROUPS, 1), jnp.float32, 0.5, 0.8))
    payload_element = payload_element + jnp.where(match_tally & gradual_shrink_factor, span_extent, jnp.float32(0.0))
    return payload_element.reshape(STREAM_NUMBER, ATTN_GROUPS * DK).astype(jnp.float32)


def shard_levels(own_key, dims, shards, low, largest):
    level, own = 1.0, jax.random.fold_in(own_key, 6)
    for position, shards_of in shards:
        heights = jnp.exp(jax.random.uniform(jax.random.fold_in(own, position), (shards_of,), jnp.float32, low / len(shards), largest / len(shards)))
        level = level * jnp.repeat(heights, dims[position] // shards_of).reshape([-1 if axis == position else 1 for axis in range(len(dims))])
    return level


def length_profile(count, total, limit, skew):
    weights = [(1 << 20) // math.isqrt(grade ** skew) + 1 for grade in range(2, count + 1)]
    rest, given = total - limit - (count - 1), [1] * (count - 1)
    while rest > 0:
        movable = [i for i in range(count - 1) if given[i] < limit]
        mass, left = sum([weights[i] for i in movable]), rest
        for i in movable:
            extra = min(limit - given[i], max(1, left * weights[i] // mass), rest)
            given[i] = given[i] + extra
            rest = rest - extra
    return np.array([limit] + given)


def uneven_parts(own_key, amount, total, limit, lean):
    if amount == 2:
        one = jax.random.randint(own_key, (), max(1, total - limit), min(limit, total - 1) + 1)
        return jnp.stack([one, total - one])
    sizes = jnp.asarray(length_profile(amount, total, limit, lean), jnp.int32)
    twos = (amount - 1) // 2
    source_of, receiver = sizes[1:1 + 2 * twos:2], sizes[2:2 + 2 * twos:2]
    slack = jnp.minimum(source_of - 1, limit - receiver)
    moved = jax.random.randint(jax.random.fold_in(own_key, 1), (twos,), 0, 1 << 20) % (slack + 1)
    sizes = sizes.at[1:1 + 2 * twos:2].set(source_of - moved).at[2:2 + 2 * twos:2].set(receiver + moved)
    return sizes[jax.random.permutation(jax.random.fold_in(own_key, 2), amount)]


def gaussian(key, extent, scale, most, cuts=(), kind=jnp.bfloat16):
    factor_of = shard_levels(key, extent, cuts, -0.22, 0.18) if cuts else 1.0
    entries = jax.random.normal(key, extent, jnp.float32) * scale * factor_of
    return jnp.minimum(jnp.maximum(entries, -most), most).astype(kind)


def setup_inputs(seed: int = 0, part: int = 0) -> dict:
    streams_of = jax.random.split(jax.random.key(seed), 20)
    part_splits = jax.random.split(jax.random.fold_in(streams_of[19], part), 20)
    return {
        "tokens": draw_tokens(jax.random.fold_in(jax.random.fold_in(streams_of[19], part), 71), part),
        "lengths": uneven_parts(part_splits[1], STREAM_NUMBER, STREAM_NUMBER * 512, min(4096, STREAM_NUMBER * 256), 2).astype(jnp.int32),
        "state": gaussian(part_splits[2], (STREAM_NUMBER, ATTN_GROUPS, DK, DV), 1.0, 6.0, ((0, 4), (1, 4)), jnp.float32),
        "key_block": gaussian(part_splits[3], (STREAM_NUMBER, ATTN_GROUPS, SPAN_STEPS, DK), 1.0, 6.0, ((0, 4), (1, 4))),
        "value_block": gaussian(part_splits[4], (STREAM_NUMBER, ATTN_GROUPS, SPAN_STEPS, DV), 1.0, 6.0, ((0, 4), (1, 4))),
        "cum_decay": draw_cum_decay(jax.random.fold_in(jax.random.fold_in(streams_of[19], part), 71), part),
        "step_decay": draw_step_decay(jax.random.fold_in(jax.random.fold_in(streams_of[19], part), 71), part),
        "g_mix": jnp.clip(1.0 + 0.18 * jax.random.normal(streams_of[7], (D,), jnp.float32), 0.099609375, 1.8984375).astype(jnp.bfloat16),
        "w_query": gaussian(streams_of[8], (D, ATTN_GROUPS * DK), D ** -0.5, 0.125, ((0, 4), (1, 4))),
        "w_key": gaussian(streams_of[9], (D, ATTN_GROUPS * DK), D ** -0.5, 0.125, ((0, 4), (1, 4))),
        "w_value": gaussian(streams_of[10], (D, ATTN_GROUPS * DV), D ** -0.5, 0.125, ((0, 4), (1, 4))),
        "w_outgate": gaussian(streams_of[11], (D, ATTN_GROUPS * DV), D ** -0.5, 0.125, ((0, 4), (1, 4))),
        "w_decay": gaussian(streams_of[12], (D, ATTN_GROUPS * DK), (D // 16) ** -0.5, 0.5, ((0, 4), (1, 4))),
        "g_heads": jnp.clip(1.0 + 0.18 * jax.random.normal(streams_of[13], (ATTN_GROUPS * DV,), jnp.float32), 0.099609375, 1.8984375).astype(jnp.bfloat16),
        "w_out": gaussian(streams_of[14], (ATTN_GROUPS * DV, D), (ATTN_GROUPS * DV) ** -0.5, 0.125, ((0, 4), (1, 4))),
        "g_ffn": jnp.clip(1.0 + 0.18 * jax.random.normal(streams_of[15], (D,), jnp.float32), 0.099609375, 1.8984375).astype(jnp.bfloat16),
        "w_gate": gaussian(streams_of[16], (D, FF), D ** -0.5, 0.125, ((0, 4), (1, 4))),
        "w_up": gaussian(streams_of[17], (D, FF), D ** -0.5, 0.125, ((0, 4), (1, 4))),
        "w_down": gaussian(streams_of[18], (FF, D), FF ** -0.5, 0.078125, ((0, 4), (1, 4))),
    }


epsilon = 1e-06
temper = 16.0

def blocked_product(left, weight):
    block_rows = left.shape[1] // N_TP
    total = jnp.zeros((left.shape[0], weight.shape[1]), jnp.float32)
    for index in range(N_TP):
        part = jnp.dot(left[:, index * block_rows:(index + 1) * block_rows], weight[index * block_rows:(index + 1) * block_rows], preferred_element_type=jnp.float32)
        rounded = lax.optimization_barrier(part.astype(jnp.bfloat16))
        total = total + rounded.astype(jnp.float32)
    return total

def reference(tokens, lengths, state, key_block, value_block, cum_decay, step_decay, g_mix, w_query, w_key, w_value, w_outgate, w_decay, g_heads, w_out, g_ffn, w_gate, w_up, w_down):
    highest = lax.Precision.HIGHEST
    inputs = tokens.astype(jnp.float32)
    inverse = lax.rsqrt(lax.optimization_barrier(jnp.sum(inputs * inputs, axis=1)) / D + epsilon)[:, None]
    scaled = (inputs * g_mix.astype(jnp.float32)).astype(jnp.bfloat16)

    def project(matrix):
        return jnp.dot(scaled, matrix, preferred_element_type=jnp.float32) * inverse
    query = (project(w_query) * DK ** (-0.5)).reshape(STREAM_NUMBER, ATTN_GROUPS, DK)
    keys_new = project(w_key).reshape(STREAM_NUMBER, ATTN_GROUPS, DK)
    values_new = project(w_value).reshape(STREAM_NUMBER, ATTN_GROUPS, DV)
    out_gate = project(w_outgate)
    decay_pre = project(w_decay)
    log_step = (jax.nn.log_sigmoid(decay_pre) / temper + step_decay).reshape(STREAM_NUMBER, ATTN_GROUPS, DK)
    live_count = lengths % SPAN_STEPS
    token_ordinal = lax.broadcasted_iota(jnp.int32, (1, 1, SPAN_STEPS, 1), 2)
    picked = jnp.where(token_ordinal == live_count[:, None, None, None] - 1, cum_decay, jnp.float32(0.0))
    token_decay = lax.optimization_barrier(jnp.sum(picked, axis=2)) + log_step
    carried = jnp.einsum('shk,shkv->shv', query * jnp.exp(token_decay), state, precision=highest)
    scores = lax.optimization_barrier(jnp.sum(query[:, :, None, :] * key_block.astype(jnp.float32) * jnp.exp(token_decay[:, :, None, :] - cum_decay), axis=3))
    scores = jnp.where(token_ordinal[..., 0] < live_count[:, None, None], scores, jnp.float32(0.0))
    in_block = jnp.einsum('shj,shjv->shv', scores, value_block.astype(jnp.float32), precision=highest)
    own_term = lax.optimization_barrier(jnp.sum(query * keys_new, axis=2))[:, :, None] * values_new
    head_out = carried + in_block + own_term
    normed = head_out * lax.rsqrt(lax.optimization_barrier(jnp.mean(head_out * head_out, axis=2, keepdims=True)) + epsilon)
    normed = normed * g_heads.astype(jnp.float32).reshape(ATTN_GROUPS, DV)
    mixed = (normed.reshape(STREAM_NUMBER, ATTN_GROUPS * DV) * jax.nn.silu(out_gate)).astype(jnp.bfloat16)
    attention = blocked_product(mixed, w_out)
    residual = (inputs + attention).astype(jnp.bfloat16)
    middle = residual.astype(jnp.float32)
    mid_inverse = lax.rsqrt(lax.optimization_barrier(jnp.sum(middle * middle, axis=1)) / D + epsilon)[:, None]
    normed_mid = (middle * g_ffn.astype(jnp.float32)).astype(jnp.bfloat16)
    gate_sum = jnp.dot(normed_mid, w_gate, preferred_element_type=jnp.float32) * mid_inverse
    up_sum = jnp.dot(normed_mid, w_up, preferred_element_type=jnp.float32) * mid_inverse
    hidden = (jax.nn.silu(gate_sum) * up_sum).astype(jnp.bfloat16)
    return (middle + blocked_product(hidden, w_down)).astype(jnp.bfloat16)
```

```python
import functools

import jax
import jax.numpy as jnp
from jax import lax
from jax.sharding import PartitionSpec as P

D = 2048
DK = 128
DV = 256


epsilon = 1e-06
temper = 16.0


def shifted(value, axis, size, shift):
    if shift % size == 0:
        return value
    return lax.ppermute(value, axis, [(i, (i + shift) % size) for i in range(size)])


def gather_relative(value, axis, size):
    return jnp.concatenate([shifted(value, axis, size, -r) for r in range(size)], axis=0)


def scatter_relative(blocks, axis, size):
    arrived = [shifted(blocks[r], axis, size, r) for r in range(size)]
    total = arrived[0].astype(jnp.float32)
    for block in arrived[1:]:
        total = total + block.astype(jnp.float32)
    return total


def sum_over(value, axis, size):
    return scatter_relative([value] * size, axis, size)


def rolled(value, start, rows):
    return lax.dynamic_slice_in_dim(jnp.concatenate([value, value], axis=0), start, rows, 0)


def body(
    sizes,
    tokens,
    lengths,
    state,
    key_block,
    value_block,
    cum_decay,
    step_decay,
    g_mix,
    w_query,
    w_key,
    w_value,
    w_outgate,
    w_decay,
    g_heads,
    w_out,
    g_ffn,
    w_gate,
    w_up,
    w_down,
):
    highest = lax.Precision.HIGHEST
    seqs = state.shape[0]
    heads = state.shape[1]
    block_len = key_block.shape[2]
    key_width = heads * DK
    value_width = heads * DV
    n_kv, n_tp = sizes
    rows = tokens.shape[0]
    place = lax.axis_index("kv")
    inputs = rolled(tokens, place * seqs, rows).astype(jnp.float32)
    square = jnp.sum(inputs * inputs, axis=1, keepdims=True)
    square_high = lax.reduce_precision(square, 8, 7)
    pad = jnp.zeros((rows, 126), jnp.float32)
    scaled = (inputs * g_mix.astype(jnp.float32)).astype(jnp.bfloat16)
    matrices = (w_query, w_key, w_value, w_outgate, w_decay)
    payload = jnp.concatenate(
        [jnp.dot(scaled, matrix, preferred_element_type=jnp.float32) for matrix in matrices]
        + [square_high, square - square_high, pad],
        axis=1,
    ).astype(jnp.bfloat16)
    payload = payload.reshape(n_kv, seqs, -1)
    projected = scatter_relative([payload[r] for r in range(n_kv)], "kv", n_kv)
    width = 3 * key_width + 2 * value_width
    own_total = projected[:, width] + projected[:, width + 1]
    projected = projected[:, :width] * lax.rsqrt(own_total / D + epsilon)[:, None]
    query = (projected[:, :key_width] * DK ** (-0.5)).reshape(seqs, heads, DK)
    keys_new = projected[:, key_width : 2 * key_width].reshape(seqs, heads, DK)
    values_new = projected[:, 2 * key_width : 2 * key_width + value_width].reshape(seqs, heads, DV)
    out_gate = projected[:, 2 * key_width + value_width : 2 * key_width + 2 * value_width]
    decay_pre = projected[:, 2 * key_width + 2 * value_width :]
    log_step = (jax.nn.log_sigmoid(decay_pre) / temper + step_decay).reshape(seqs, heads, DK)
    live_count = lengths % block_len
    token_ordinal = lax.broadcasted_iota(jnp.int32, (1, 1, block_len, 1), 2)
    picked = jnp.where(
        token_ordinal == live_count[:, None, None, None] - 1, cum_decay, jnp.float32(0.0)
    )
    token_decay = jnp.sum(picked, axis=2) + log_step
    carried = jnp.einsum("shk,shkv->shv", query * jnp.exp(token_decay), state, precision=highest)
    scores = jnp.sum(
        query[:, :, None, :]
        * key_block.astype(jnp.float32)
        * jnp.exp(token_decay[:, :, None, :] - cum_decay),
        axis=3,
    )
    scores = jnp.where(token_ordinal[..., 0] < live_count[:, None, None], scores, jnp.float32(0.0))
    in_block = jnp.einsum(
        "shj,shjv->shv", scores, value_block.astype(jnp.float32), precision=highest
    )
    own_term = jnp.sum(query * keys_new, axis=2)[:, :, None] * values_new
    head_out = carried + in_block + own_term
    normed = head_out * lax.rsqrt(jnp.mean(head_out * head_out, axis=2, keepdims=True) + epsilon)
    normed = normed * g_heads.astype(jnp.float32).reshape(heads, DV)
    mixed = (normed.reshape(seqs, value_width) * jax.nn.silu(out_gate)).astype(jnp.bfloat16)
    attn_part = jnp.dot(
        gather_relative(mixed, "kv", n_kv), w_out, preferred_element_type=jnp.float32
    ).astype(jnp.bfloat16)
    attention = sum_over(attn_part, "tp", n_tp)
    residual = (inputs + attention).astype(jnp.bfloat16)
    middle = residual.astype(jnp.float32)
    square_mid = jnp.sum(middle * middle, axis=1, keepdims=True)
    mid_high = lax.reduce_precision(square_mid, 8, 7)
    normed_mid = (middle * g_ffn.astype(jnp.float32)).astype(jnp.bfloat16)
    units = w_gate.shape[1]
    payload_mid = jnp.concatenate(
        [
            jnp.dot(normed_mid, w_gate, preferred_element_type=jnp.float32),
            jnp.dot(normed_mid, w_up, preferred_element_type=jnp.float32),
            mid_high,
            square_mid - mid_high,
            pad,
        ],
        axis=1,
    ).astype(jnp.bfloat16)
    payload_mid = payload_mid.reshape(n_kv, seqs, -1)
    sums = scatter_relative([payload_mid[r] for r in range(n_kv)], "kv", n_kv)
    mid_total = sums[:, 2 * units] + sums[:, 2 * units + 1]
    mid_inverse = lax.rsqrt(mid_total / D + epsilon)[:, None]
    gate_sum = sums[:, :units] * mid_inverse
    up_sum = sums[:, units : 2 * units] * mid_inverse
    hidden = (jax.nn.silu(gate_sum) * up_sum).astype(jnp.bfloat16)
    down_part = jnp.dot(
        gather_relative(hidden, "kv", n_kv), w_down, preferred_element_type=jnp.float32
    ).astype(jnp.bfloat16)
    updated = (middle + sum_over(down_part, "tp", n_tp)).astype(jnp.bfloat16)
    return rolled(updated, (n_kv - place) % n_kv * seqs, rows)


def solution(mesh):
    sizes = (mesh.shape["kv"], mesh.shape["tp"])
    return jax.shard_map(
        functools.partial(body, sizes),
        mesh=mesh,
        in_specs=(
            P("grp", "kv"),
            P(("grp", "kv")),
            P(("grp", "kv"), "tp", None, None),
            P(("grp", "kv"), "tp", None, None),
            P(("grp", "kv"), "tp", None, None),
            P(("grp", "kv"), "tp", None, None),
            P(("grp", "kv"), "tp"),
            P("kv"),
            P("kv", "tp"),
            P("kv", "tp"),
            P("kv", "tp"),
            P("kv", "tp"),
            P("kv", "tp"),
            P("tp"),
            P("tp", "kv"),
            P("kv"),
            P("kv", "tp"),
            P("kv", "tp"),
            P("tp", "kv"),
        ),
        out_specs=P("grp", "kv"),
        check_vma=False,
    )
```

```python
import functools

import jax
import jax.numpy as jnp
from jax import lax
from jax.experimental import pallas as pl
from jax.experimental.pallas import tpu as pltpu
from jax.sharding import PartitionSpec as P

D = 2048
DK = 128
DV = 256
LANES = 128


epsilon = 1e-06
temper = 16.0

f32 = jnp.float32
bf16 = jnp.bfloat16


def swapped(value, axis, size, mask):
    return lax.ppermute(value, axis, [(i, i ^ mask) for i in range(size)])


def pair_sum(values):
    while len(values) > 1:
        values = [values[i] + values[i + 1] for i in range(0, len(values), 2)]
    return values[0]


def call(kernel, outs, scalars, args, vmem=24, scratch=()):
    specs = [pl.BlockSpec(memory_space=pltpu.SMEM)] * len(scalars)
    specs += [pl.BlockSpec(memory_space=pltpu.VMEM)] * len(args)
    return pl.pallas_call(
        kernel,
        out_shape=[jax.ShapeDtypeStruct(shape, kind) for shape, kind in outs],
        in_specs=specs,
        out_specs=[pl.BlockSpec(memory_space=pltpu.VMEM)] * len(outs),
        scratch_shapes=list(scratch),
        compiler_params=pltpu.CompilerParams(vmem_limit_bytes=vmem << 20),
    )(*scalars, *args)


def put_with_squares(out_refs, seqs, parts, square):
    high = square.astype(bf16).astype(f32)
    lane = lax.broadcasted_iota(jnp.int32, (square.shape[0], LANES), 1)
    tail = jnp.where(lane == 0, high, jnp.where(lane == 1, square - high, f32(0.0))).astype(bf16)
    width = out_refs[0].shape[1] - LANES
    for r, out in enumerate(out_refs):
        out[:, width:] = tail[r * seqs : (r + 1) * seqs]
    column = 0
    for left, ref in parts:
        product = jnp.dot(left, ref[...], preferred_element_type=f32).astype(bf16)
        for r, out in enumerate(out_refs):
            out[:, column : column + product.shape[1]] = product[r * seqs : (r + 1) * seqs]
        column += product.shape[1]


def project_kernel(n_kv, seqs, place_ref, tokens, gain, *refs):
    matrices, outs = refs[:5], refs[5:]
    place = place_ref[0]
    inputs = jnp.concatenate(
        [tokens[pl.ds(pl.multiple_of((place ^ r) * seqs, seqs), seqs), :] for r in range(n_kv)],
        axis=0,
    ).astype(f32)
    scaled = (inputs * gain[...].astype(f32)).astype(bf16)
    square = jnp.sum(inputs * inputs, axis=1, keepdims=True)
    put_with_squares(outs, seqs, [(scaled, ref) for ref in matrices], square)


def sums_of(parts):
    return pair_sum([part.astype(f32) for part in parts])


def attend_kernel(n_kv, lengths, state, keys, values, cum_decay, step_decay, gain, *refs):
    parts, out, rows_ref = refs[:n_kv], refs[n_kv], refs[n_kv + 1]
    seqs, heads, block_len = keys.shape[0], keys.shape[1], keys.shape[2]
    kw, vw = heads * DK, heads * DV
    width = 3 * kw + 2 * vw
    tail = sums_of([part[:, width:] for part in parts])
    inverse = lax.rsqrt((tail[:, 0:1] + tail[:, 1:2]) / D + epsilon)

    def taken(start, size):
        return sums_of([part[:, start : start + size] for part in parts]) * inverse

    step = jax.nn.log_sigmoid(taken(2 * kw + 2 * vw, kw)) / temper + step_decay[...]
    order = lax.broadcasted_iota(jnp.int32, (block_len, 1), 0)
    for h in range(heads):
        query = taken(h * DK, DK) * DK ** (-0.5)
        key_new = taken(kw + h * DK, DK)
        value_new = taken(2 * kw + h * DV, DV)
        gate = taken(2 * kw + vw + h * DV, DV)
        decay_rows = []
        for s in range(seqs):
            live = lengths[s] % block_len
            picked = jnp.where(order == live - 1, cum_decay[s, h], f32(0.0))
            decay_rows.append(jnp.sum(picked, axis=0, keepdims=True))
        decay = jnp.concatenate(decay_rows, axis=0) + step[:, h * DK : (h + 1) * DK]
        carry = jnp.transpose(query * jnp.exp(decay))
        for s in range(seqs):
            live = lengths[s] % block_len
            weight = jnp.exp(decay[s : s + 1] - cum_decay[s, h]) * keys[s, h].astype(f32)
            scores = jnp.sum(query[s : s + 1] * weight, axis=1, keepdims=True)
            scores = jnp.where(order < live, scores, f32(0.0))
            in_block = jnp.sum(scores * values[s, h].astype(f32), axis=0, keepdims=True)
            carried = jnp.sum(carry[:, s : s + 1] * state[s, h], axis=0, keepdims=True)
            rows_ref[s : s + 1, :] = carried + in_block
        head = rows_ref[...] + jnp.sum(query * key_new, axis=1, keepdims=True) * value_new
        head = head * lax.rsqrt(jnp.mean(head * head, axis=1, keepdims=True) + epsilon)
        columns = slice(h * DV, (h + 1) * DV)
        head = head * gain[:, columns].astype(f32)
        out[:, columns] = (head * (gate / (1.0 + jnp.exp(-gate)))).astype(bf16)


def dot_kernel(*refs):
    blocks, matrix, out = refs[:-2], refs[-2], refs[-1]
    left = jnp.concatenate([block[...] for block in blocks], axis=0)
    out[...] = jnp.dot(left, matrix[...], preferred_element_type=f32).astype(bf16)


def mix_kernel(n_kv, n_parts, seqs, place_ref, tokens, gain, w_gate, w_up, *refs):
    parts, residual_ref, outs = refs[:n_parts], refs[n_parts], refs[n_parts + 1 :]
    place = place_ref[0]
    inputs = jnp.concatenate(
        [tokens[pl.ds(pl.multiple_of((place ^ r) * seqs, seqs), seqs), :] for r in range(n_kv)],
        axis=0,
    ).astype(f32)
    residual = (inputs + sums_of([part[...] for part in parts])).astype(bf16)
    residual_ref[...] = residual
    middle = residual.astype(f32)
    normed = (middle * gain[...].astype(f32)).astype(bf16)
    square = jnp.sum(middle * middle, axis=1, keepdims=True)
    put_with_squares(outs, seqs, [(normed, w_gate), (normed, w_up)], square)


def hidden_kernel(*refs):
    parts, out = refs[:-1], refs[-1]
    units = out.shape[1]
    tail = sums_of([part[:, 2 * units :] for part in parts])
    inverse = lax.rsqrt((tail[:, 0:1] + tail[:, 1:2]) / D + epsilon)
    gate = sums_of([part[:, :units] for part in parts]) * inverse
    up = sums_of([part[:, units : 2 * units] for part in parts]) * inverse
    out[...] = (gate / (1.0 + jnp.exp(-gate)) * up).astype(bf16)


def finish_kernel(n_kv, seqs, place_ref, residual, *refs):
    parts, out = refs[:-1], refs[-1]
    place = place_ref[0]
    total = residual[...].astype(f32) + sums_of([part[...] for part in parts])
    total = total.astype(bf16)
    for r in range(n_kv):
        out[pl.ds(pl.multiple_of((place ^ r) * seqs, seqs), seqs), :] = total[
            r * seqs : (r + 1) * seqs
        ]


def partials_direct(value, axis, size):
    return [value] + [swapped(value, axis, size, r) for r in range(1, size)]


def partials_tree(value, axis, size):
    mask = 1
    while 2 * mask < size:
        other = swapped(value, axis, size, mask)
        value = (value.astype(f32) + other.astype(f32)).astype(bf16)
        mask *= 2
    return [value, swapped(value, axis, size, mask)]


def body(
    sizes,
    tokens,
    lengths,
    state,
    key_block,
    value_block,
    cum_decay,
    step_decay,
    g_mix,
    w_query,
    w_key,
    w_value,
    w_outgate,
    w_decay,
    g_heads,
    w_out,
    g_ffn,
    w_gate,
    w_up,
    w_down,
):
    n_kv, n_tp = sizes
    seqs, heads = state.shape[0], state.shape[1]
    rows, columns = tokens.shape
    units = w_gate.shape[1]
    place = lax.axis_index("kv").astype(jnp.int32)[None]
    width = 3 * heads * DK + 2 * heads * DV + LANES
    blocks = call(
        functools.partial(project_kernel, n_kv, seqs),
        [((seqs, width), bf16)] * n_kv,
        [place],
        [tokens, g_mix[None], w_query, w_key, w_value, w_outgate, w_decay],
    )
    arrived = [blocks[0]] + [swapped(blocks[r], "kv", n_kv, r) for r in range(1, n_kv)]
    (mixed,) = call(
        functools.partial(attend_kernel, n_kv),
        [((seqs, heads * DV), bf16)],
        [lengths],
        [state, key_block, value_block, cum_decay, step_decay, g_heads[None], *arrived],
        scratch=[pltpu.VMEM((seqs, DV), f32)],
    )
    (attn_part,) = call(
        dot_kernel,
        [((rows, w_out.shape[1]), bf16)],
        [],
        [*partials_direct(mixed, "kv", n_kv), w_out],
    )
    attn_parts = partials_direct(attn_part, "tp", n_tp)
    residual, *blocks = call(
        functools.partial(mix_kernel, n_kv, len(attn_parts), seqs),
        [((rows, columns), bf16)] + [((seqs, 2 * units + LANES), bf16)] * n_kv,
        [place],
        [tokens, g_ffn[None], w_gate, w_up, *attn_parts],
    )
    arrived = [blocks[0]] + [swapped(blocks[r], "kv", n_kv, r) for r in range(1, n_kv)]
    (hidden,) = call(hidden_kernel, [((seqs, units), bf16)], [], arrived)
    (down_part,) = call(
        dot_kernel,
        [((rows, w_down.shape[1]), bf16)],
        [],
        [*partials_direct(hidden, "kv", n_kv), w_down],
    )
    (updated,) = call(
        functools.partial(finish_kernel, n_kv, seqs),
        [((rows, columns), bf16)],
        [place],
        [residual, *partials_tree(down_part, "tp", n_tp)],
    )
    return updated


def solution(mesh):
    sizes = (mesh.shape["kv"], mesh.shape["tp"])
    return jax.shard_map(
        functools.partial(body, sizes),
        mesh=mesh,
        in_specs=(
            P("grp", "kv"),
            P(("grp", "kv")),
            P(("grp", "kv"), "tp", None, None),
            P(("grp", "kv"), "tp", None, None),
            P(("grp", "kv"), "tp", None, None),
            P(("grp", "kv"), "tp", None, None),
            P(("grp", "kv"), "tp"),
            P("kv"),
            P("kv", "tp"),
            P("kv", "tp"),
            P("kv", "tp"),
            P("kv", "tp"),
            P("kv", "tp"),
            P("tp"),
            P("tp", "kv"),
            P("kv"),
            P("kv", "tp"),
            P("kv", "tp"),
            P("tp", "kv"),
        ),
        out_specs=P("grp", "kv"),
        check_vma=False,
    )
```

```python
import functools

import jax
import jax.numpy as jnp
from jax import lax
from jax.experimental import pallas as pl
from jax.experimental.pallas import tpu as pltpu
from jax.sharding import PartitionSpec as P

D = 2048
DK = 128
DV = 256
LANES = 128


epsilon = 1e-06
temper = 16.0

f32 = jnp.float32
bf16 = jnp.bfloat16


def swapped(value, axis, size, mask):
    return lax.ppermute(value, axis, [(i, i ^ mask) for i in range(size)])


def pair_sum(values):
    while len(values) > 1:
        values = [values[i] + values[i + 1] for i in range(0, len(values), 2)]
    return values[0]


def call(kernel, outs, scalars, args, vmem=24576, scratch=(), far=0, cost=None):
    specs = [pl.BlockSpec(memory_space=pltpu.SMEM)] * len(scalars)
    specs += [pl.BlockSpec(memory_space=pltpu.VMEM)] * (len(args) - far)
    specs += [pl.BlockSpec(memory_space=pltpu.HBM)] * far
    return pl.pallas_call(
        kernel,
        out_shape=[jax.ShapeDtypeStruct(shape, kind) for shape, kind in outs],
        in_specs=specs,
        out_specs=[pl.BlockSpec(memory_space=pltpu.VMEM)] * len(outs),
        scratch_shapes=list(scratch),
        cost_estimate=cost,
        compiler_params=pltpu.CompilerParams(vmem_limit_bytes=vmem << 10),
    )(*scalars, *args)


def put_with_squares(out_refs, seqs, parts, square):
    high = square.astype(bf16).astype(f32)
    lane = lax.broadcasted_iota(jnp.int32, (square.shape[0], LANES), 1)
    tail = jnp.where(lane == 0, high, jnp.where(lane == 1, square - high, f32(0.0))).astype(bf16)
    width = out_refs[0].shape[1] - LANES
    for r, out in enumerate(out_refs):
        out[:, width:] = tail[r * seqs : (r + 1) * seqs]
    column = 0
    for left, ref in parts:
        product = jnp.dot(left, ref[...], preferred_element_type=f32).astype(bf16)
        for r, out in enumerate(out_refs):
            out[:, column : column + product.shape[1]] = product[r * seqs : (r + 1) * seqs]
        column += product.shape[1]


def project_kernel(n_kv, seqs, place_ref, gain, *refs):
    far, outs, near, sems = refs[:6], refs[6 : 6 + n_kv], refs[6 + n_kv : 12 + n_kv], refs[-1]
    copies = [pltpu.make_async_copy(far[i], near[i], sems.at[i]) for i in range(6)]
    for copy in copies:
        copy.start()
    for copy in copies:
        copy.wait()
    tokens, matrices = near[0], near[1:]
    place = place_ref[0]
    inputs = jnp.concatenate(
        [tokens[pl.ds(pl.multiple_of((place ^ r) * seqs, seqs), seqs), :] for r in range(n_kv)],
        axis=0,
    ).astype(f32)
    scaled = (inputs * gain[...].astype(f32)).astype(bf16)
    square = jnp.sum(inputs * inputs, axis=1, keepdims=True)
    put_with_squares(outs, seqs, [(scaled, ref) for ref in matrices], square)


def fetch_kernel(*refs):
    count = (len(refs) - 1) // 2
    copies = [
        pltpu.make_async_copy(refs[i], refs[count + i], refs[-1].at[i]) for i in range(count)
    ]
    for copy in copies:
        copy.start()
    for copy in copies:
        copy.wait()


def sums_of(parts):
    return pair_sum([part.astype(f32) for part in parts])


def attend_kernel(n_kv, lengths, state, keys, values, cum_decay, step_decay, gain, *refs):
    parts, out, rows_ref = refs[:n_kv], refs[n_kv], refs[n_kv + 1]
    seqs, heads, block_len = keys.shape[0], keys.shape[1], keys.shape[2]
    kw, vw = heads * DK, heads * DV
    width = 3 * kw + 2 * vw
    tail = sums_of([part[:, width:] for part in parts])
    inverse = lax.rsqrt((tail[:, 0:1] + tail[:, 1:2]) / D + epsilon)

    def taken(start, size):
        return sums_of([part[:, start : start + size] for part in parts]) * inverse

    step = jax.nn.log_sigmoid(taken(2 * kw + 2 * vw, kw)) / temper + step_decay[...]
    order = lax.broadcasted_iota(jnp.int32, (block_len, 1), 0)
    for h in range(heads):
        query = taken(h * DK, DK) * DK ** (-0.5)
        key_new = taken(kw + h * DK, DK)
        value_new = taken(2 * kw + h * DV, DV)
        gate = taken(2 * kw + vw + h * DV, DV)
        decay_rows = []
        for s in range(seqs):
            live = lengths[s] % block_len
            picked = jnp.where(order == live - 1, cum_decay[s, h], f32(0.0))
            decay_rows.append(jnp.sum(picked, axis=0, keepdims=True))
        decay = jnp.concatenate(decay_rows, axis=0) + step[:, h * DK : (h + 1) * DK]
        carry = jnp.transpose(query * jnp.exp(decay))
        for s in range(seqs):
            live = lengths[s] % block_len
            weight = jnp.exp(decay[s : s + 1] - cum_decay[s, h]) * keys[s, h].astype(f32)
            scores = jnp.sum(query[s : s + 1] * weight, axis=1, keepdims=True)
            scores = jnp.where(order < live, scores, f32(0.0))
            in_block = jnp.sum(scores * values[s, h].astype(f32), axis=0, keepdims=True)
            carried = jnp.sum(carry[:, s : s + 1] * state[s, h], axis=0, keepdims=True)
            rows_ref[s : s + 1, :] = carried + in_block
        head = rows_ref[...] + jnp.sum(query * key_new, axis=1, keepdims=True) * value_new
        head = head * lax.rsqrt(jnp.mean(head * head, axis=1, keepdims=True) + epsilon)
        columns = slice(h * DV, (h + 1) * DV)
        head = head * gain[:, columns].astype(f32)
        out[:, columns] = (head * (gate / (1.0 + jnp.exp(-gate)))).astype(bf16)


def dot_kernel(*refs):
    blocks, matrix, out = refs[:-2], refs[-2], refs[-1]
    left = jnp.concatenate([block[...] for block in blocks], axis=0)
    out[...] = jnp.dot(left, matrix[...], preferred_element_type=f32).astype(bf16)


def mix_kernel(n_kv, n_parts, seqs, place_ref, tokens, gain, w_gate, w_up, *refs):
    parts, residual_ref, outs = refs[:n_parts], refs[n_parts], refs[n_parts + 1 :]
    place = place_ref[0]
    inputs = jnp.concatenate(
        [tokens[pl.ds(pl.multiple_of((place ^ r) * seqs, seqs), seqs), :] for r in range(n_kv)],
        axis=0,
    ).astype(f32)
    residual = (inputs + sums_of([part[...] for part in parts])).astype(bf16)
    residual_ref[...] = residual
    middle = residual.astype(f32)
    normed = (middle * gain[...].astype(f32)).astype(bf16)
    square = jnp.sum(middle * middle, axis=1, keepdims=True)
    put_with_squares(outs, seqs, [(normed, w_gate), (normed, w_up)], square)


def hidden_kernel(*refs):
    parts, out = refs[:-1], refs[-1]
    units = out.shape[1]
    tail = sums_of([part[:, 2 * units :] for part in parts])
    inverse = lax.rsqrt((tail[:, 0:1] + tail[:, 1:2]) / D + epsilon)
    gate = sums_of([part[:, :units] for part in parts]) * inverse
    up = sums_of([part[:, units : 2 * units] for part in parts]) * inverse
    out[...] = (gate / (1.0 + jnp.exp(-gate)) * up).astype(bf16)


def finish_kernel(n_kv, seqs, place_ref, residual, *refs):
    parts, out = refs[:-1], refs[-1]
    place = place_ref[0]
    total = residual[...].astype(f32) + sums_of([part[...] for part in parts])
    total = total.astype(bf16)
    for r in range(n_kv):
        out[pl.ds(pl.multiple_of((place ^ r) * seqs, seqs), seqs), :] = total[
            r * seqs : (r + 1) * seqs
        ]


def partials_direct(value, axis, size):
    return [value] + [swapped(value, axis, size, r) for r in range(1, size)]


def partials_tree(value, axis, size):
    mask = 1
    while 2 * mask < size:
        other = swapped(value, axis, size, mask)
        value = (value.astype(f32) + other.astype(f32)).astype(bf16)
        mask *= 2
    return [value, swapped(value, axis, size, mask)]


def body(
    sizes,
    tokens,
    lengths,
    state,
    key_block,
    value_block,
    cum_decay,
    step_decay,
    g_mix,
    w_query,
    w_key,
    w_value,
    w_outgate,
    w_decay,
    g_heads,
    w_out,
    g_ffn,
    w_gate,
    w_up,
    w_down,
):
    n_kv, n_tp = sizes
    seqs, heads = state.shape[0], state.shape[1]
    rows, columns = tokens.shape
    units = w_gate.shape[1]
    place = lax.axis_index("kv").astype(jnp.int32)[None]
    width = 3 * heads * DK + 2 * heads * DV + LANES
    first = (tokens, w_query, w_key, w_value, w_outgate, w_decay)
    blocks = call(
        functools.partial(project_kernel, n_kv, seqs),
        [((seqs, width), bf16)] * n_kv,
        [place],
        [g_mix[None], *first],
        scratch=[pltpu.VMEM(array.shape, array.dtype) for array in first]
        + [pltpu.SemaphoreType.DMA((len(first),))],
        far=len(first),
        vmem=54988,
    )
    arrived = [blocks[0]] + [swapped(blocks[r], "kv", n_kv, r) for r in range(1, n_kv)]
    held = (state,)
    with jax.named_scope("fetch"):
        (state,) = call(
            fetch_kernel,
            [(array.shape, array.dtype) for array in held],
            [],
            held,
            scratch=[pltpu.SemaphoreType.DMA((len(held),))],
            far=len(held),
            vmem=48128,
            cost=pl.CostEstimate(flops=10**8, transcendentals=0, bytes_accessed=14 << 20),
        )
    (mixed,) = call(
        functools.partial(attend_kernel, n_kv),
        [((seqs, heads * DV), bf16)],
        [lengths],
        [state, key_block, value_block, cum_decay, step_decay, g_heads[None], *arrived],
        scratch=[pltpu.VMEM((seqs, DV), f32)],
    )
    (attn_part,) = call(
        dot_kernel,
        [((rows, w_out.shape[1]), bf16)],
        [],
        [*partials_direct(mixed, "kv", n_kv), w_out],
    )
    attn_parts = partials_tree(attn_part, "tp", n_tp)
    residual, *blocks = call(
        functools.partial(mix_kernel, n_kv, len(attn_parts), seqs),
        [((rows, columns), bf16)] + [((seqs, 2 * units + LANES), bf16)] * n_kv,
        [place],
        [tokens, g_ffn[None], w_gate, w_up, *attn_parts],
    )
    arrived = [blocks[0]] + [swapped(blocks[r], "kv", n_kv, r) for r in range(1, n_kv)]
    (hidden,) = call(hidden_kernel, [((seqs, units), bf16)], [], arrived)
    (down_part,) = call(
        dot_kernel,
        [((rows, w_down.shape[1]), bf16)],
        [],
        [*partials_direct(hidden, "kv", n_kv), w_down],
    )
    (updated,) = call(
        functools.partial(finish_kernel, n_kv, seqs),
        [((rows, columns), bf16)],
        [place],
        [residual, *partials_tree(down_part, "tp", n_tp)],
    )
    return updated


def solution(mesh):
    sizes = (mesh.shape["kv"], mesh.shape["tp"])
    return jax.shard_map(
        functools.partial(body, sizes),
        mesh=mesh,
        in_specs=(
            P("grp", "kv"),
            P(("grp", "kv")),
            P(("grp", "kv"), "tp", None, None),
            P(("grp", "kv"), "tp", None, None),
            P(("grp", "kv"), "tp", None, None),
            P(("grp", "kv"), "tp", None, None),
            P(("grp", "kv"), "tp"),
            P("kv"),
            P("kv", "tp"),
            P("kv", "tp"),
            P("kv", "tp"),
            P("kv", "tp"),
            P("kv", "tp"),
            P("tp"),
            P("tp", "kv"),
            P("kv"),
            P("kv", "tp"),
            P("kv", "tp"),
            P("tp", "kv"),
        ),
        out_specs=P("grp", "kv"),
        check_vma=False,
    )
```

```python
import functools

import jax
import jax.numpy as jnp
from jax import lax
from jax.experimental import pallas as pl
from jax.experimental.pallas import tpu as pltpu
from jax.sharding import PartitionSpec as P

D = 2048
DK = 128
DV = 256
LANES = 128


epsilon = 1e-06
temper = 16.0

f32 = jnp.float32
bf16 = jnp.bfloat16


def swapped(value, axis, size, mask):
    return lax.ppermute(value, axis, [(i, i ^ mask) for i in range(size)])


def pair_sum(values):
    while len(values) > 1:
        values = [values[i] + values[i + 1] for i in range(0, len(values), 2)]
    return values[0]


def call(kernel, outs, scalars, args, vmem=24576, scratch=(), far=0, cost=None):
    specs = [pl.BlockSpec(memory_space=pltpu.SMEM)] * len(scalars)
    specs += [pl.BlockSpec(memory_space=pltpu.VMEM)] * (len(args) - far)
    specs += [pl.BlockSpec(memory_space=pltpu.HBM)] * far
    return pl.pallas_call(
        kernel,
        out_shape=[jax.ShapeDtypeStruct(shape, kind) for shape, kind in outs],
        in_specs=specs,
        out_specs=[pl.BlockSpec(memory_space=pltpu.VMEM)] * len(outs),
        scratch_shapes=list(scratch),
        cost_estimate=cost,
        compiler_params=pltpu.CompilerParams(vmem_limit_bytes=vmem << 10),
    )(*scalars, *args)


def put_with_squares(out_refs, seqs, parts, square):
    high = square.astype(bf16).astype(f32)
    lane = lax.broadcasted_iota(jnp.int32, (square.shape[0], LANES), 1)
    tail = jnp.where(lane == 0, high, jnp.where(lane == 1, square - high, f32(0.0))).astype(bf16)
    width = out_refs[0].shape[1] - LANES
    for r, out in enumerate(out_refs):
        out[:, width:] = tail[r * seqs : (r + 1) * seqs]
    column = 0
    for left, ref in parts:
        product = jnp.dot(left, ref[...], preferred_element_type=f32).astype(bf16)
        for r, out in enumerate(out_refs):
            out[:, column : column + product.shape[1]] = product[r * seqs : (r + 1) * seqs]
        column += product.shape[1]


def project_kernel(n_kv, seqs, place_ref, gain, *refs):
    far, outs, near, sems = refs[:6], refs[6 : 6 + n_kv], refs[6 + n_kv : 12 + n_kv], refs[-1]
    copies = [pltpu.make_async_copy(far[i], near[i], sems.at[i]) for i in range(6)]
    for copy in copies:
        copy.start()
    for copy in copies:
        copy.wait()
    tokens, matrices = near[0], near[1:]
    place = place_ref[0]
    inputs = jnp.concatenate(
        [tokens[pl.ds(pl.multiple_of((place ^ r) * seqs, seqs), seqs), :] for r in range(n_kv)],
        axis=0,
    ).astype(f32)
    scaled = (inputs * gain[...].astype(f32).reshape(1, -1)).astype(bf16)
    square = jnp.sum(inputs * inputs, axis=1, keepdims=True)
    put_with_squares(outs, seqs, [(scaled, ref) for ref in matrices], square)


def fetch_kernel(*refs):
    count = (len(refs) - 1) // 2
    copies = [
        pltpu.make_async_copy(refs[i], refs[count + i], refs[-1].at[i]) for i in range(count)
    ]
    for copy in copies:
        copy.start()
    for copy in copies:
        copy.wait()


def sums_of(parts):
    return pair_sum([part.astype(f32) for part in parts])


def attend_kernel(n_kv, lengths, state, keys, values, cum_decay, step_decay, gain, *refs):
    parts, out, rows_ref = refs[:n_kv], refs[n_kv], refs[n_kv + 1]
    seqs, heads, block_len = keys.shape[0], keys.shape[1], keys.shape[2]
    kw, vw = heads * DK, heads * DV
    width = 3 * kw + 2 * vw
    tail = sums_of([part[:, width:] for part in parts])
    inverse = lax.rsqrt((tail[:, 0:1] + tail[:, 1:2]) / D + epsilon)

    def taken(start, size):
        return sums_of([part[:, start : start + size] for part in parts]) * inverse

    step = jax.nn.log_sigmoid(taken(2 * kw + 2 * vw, kw)) / temper + step_decay[...]
    order = lax.broadcasted_iota(jnp.int32, (block_len, 1), 0)
    for h in range(heads):
        query = taken(h * DK, DK) * DK ** (-0.5)
        key_new = taken(kw + h * DK, DK)
        value_new = taken(2 * kw + h * DV, DV)
        gate = taken(2 * kw + vw + h * DV, DV)
        decay_rows = []
        for s in range(seqs):
            live = lengths[s] % block_len
            picked = jnp.where(order == live - 1, cum_decay[s, h], f32(0.0))
            decay_rows.append(jnp.sum(picked, axis=0, keepdims=True))
        decay = jnp.concatenate(decay_rows, axis=0) + step[:, h * DK : (h + 1) * DK]
        carry = jnp.transpose(query * jnp.exp(decay))
        for s in range(seqs):
            live = lengths[s] % block_len
            weight = jnp.exp(decay[s : s + 1] - cum_decay[s, h]) * keys[s, h].astype(f32)
            scores = jnp.sum(query[s : s + 1] * weight, axis=1, keepdims=True)
            scores = jnp.where(order < live, scores, f32(0.0))
            in_block = jnp.sum(scores * values[s, h].astype(f32), axis=0, keepdims=True)
            carried = jnp.sum(carry[:, s : s + 1] * state[s, h], axis=0, keepdims=True)
            rows_ref[s : s + 1, :] = carried + in_block
        head = rows_ref[...] + jnp.sum(query * key_new, axis=1, keepdims=True) * value_new
        head = head * lax.rsqrt(jnp.mean(head * head, axis=1, keepdims=True) + epsilon)
        columns = slice(h * DV, (h + 1) * DV)
        head = head * gain[:, columns].astype(f32)
        out[:, columns] = (head * (gate / (1.0 + jnp.exp(-gate)))).astype(bf16)


def dot_kernel(*refs):
    blocks, matrix, out = refs[:-2], refs[-2], refs[-1]
    left = jnp.concatenate([block[...] for block in blocks], axis=0)
    out[...] = jnp.dot(left, matrix[...], preferred_element_type=f32).astype(bf16)


def mix_kernel(n_kv, n_parts, seqs, place_ref, tokens, gain, w_gate, w_up, *refs):
    parts, residual_ref, outs = refs[:n_parts], refs[n_parts], refs[n_parts + 1 :]
    place = place_ref[0]
    inputs = jnp.concatenate(
        [tokens[pl.ds(pl.multiple_of((place ^ r) * seqs, seqs), seqs), :] for r in range(n_kv)],
        axis=0,
    ).astype(f32)
    residual = (inputs + sums_of([part[...] for part in parts])).astype(bf16)
    residual_ref[...] = residual
    middle = residual.astype(f32)
    normed = (middle * gain[...].astype(f32)).astype(bf16)
    square = jnp.sum(middle * middle, axis=1, keepdims=True)
    put_with_squares(outs, seqs, [(normed, w_gate), (normed, w_up)], square)


def hidden_kernel(*refs):
    parts, out = refs[:-1], refs[-1]
    units = out.shape[1]
    tail = sums_of([part[:, 2 * units :] for part in parts])
    inverse = lax.rsqrt((tail[:, 0:1] + tail[:, 1:2]) / D + epsilon)
    gate = sums_of([part[:, :units] for part in parts]) * inverse
    up = sums_of([part[:, units : 2 * units] for part in parts]) * inverse
    out[...] = (gate / (1.0 + jnp.exp(-gate)) * up).astype(bf16)


def finish_kernel(n_kv, seqs, place_ref, residual, *refs):
    parts, out = refs[:-1], refs[-1]
    place = place_ref[0]
    total = residual[...].astype(f32) + sums_of([part[...] for part in parts])
    total = total.astype(bf16)
    for r in range(n_kv):
        out[pl.ds(pl.multiple_of((place ^ r) * seqs, seqs), seqs), :] = total[
            r * seqs : (r + 1) * seqs
        ]


def partials_direct(value, axis, size):
    return [value] + [swapped(value, axis, size, r) for r in range(1, size)]


def gathered_tree(value, axis, size):
    mask = 1
    while 2 * mask < size:
        value = jnp.concatenate([value, swapped(value, axis, size, mask)], axis=0)
        mask *= 2
    return value


def partials_tree(value, axis, size):
    mask = 1
    while 2 * mask < size:
        other = swapped(value, axis, size, mask)
        value = (value.astype(f32) + other.astype(f32)).astype(bf16)
        mask *= 2
    return [value, swapped(value, axis, size, mask)]


def body(
    sizes,
    tokens,
    lengths,
    state,
    key_block,
    value_block,
    cum_decay,
    step_decay,
    g_mix,
    w_query,
    w_key,
    w_value,
    w_outgate,
    w_decay,
    g_heads,
    w_out,
    g_ffn,
    w_gate,
    w_up,
    w_down,
):
    n_kv, n_tp = sizes
    seqs, heads = state.shape[0], state.shape[1]
    rows, columns = tokens.shape
    units = w_gate.shape[1]
    place = lax.axis_index("kv").astype(jnp.int32)[None]
    width = 3 * heads * DK + 2 * heads * DV + LANES
    first = (tokens, w_query, w_key, w_value, w_outgate, w_decay)
    blocks = call(
        functools.partial(project_kernel, n_kv, seqs),
        [((seqs, width), bf16)] * n_kv,
        [place],
        [g_mix, *first],
        scratch=[pltpu.VMEM(array.shape, array.dtype) for array in first]
        + [pltpu.SemaphoreType.DMA((len(first),))],
        far=len(first),
        vmem=54960,
    )
    arrived = [blocks[0]] + [swapped(blocks[r], "kv", n_kv, r) for r in range(1, n_kv)]
    held = (state,)
    with jax.named_scope("fetch"):
        (state,) = call(
            fetch_kernel,
            [(array.shape, array.dtype) for array in held],
            [],
            held,
            scratch=[pltpu.SemaphoreType.DMA((len(held),))],
            far=len(held),
            vmem=48128,
            cost=pl.CostEstimate(flops=10**8, transcendentals=0, bytes_accessed=14 << 20),
        )
    (mixed,) = call(
        functools.partial(attend_kernel, n_kv),
        [((seqs, heads * DV), bf16)],
        [lengths],
        [state, key_block, value_block, cum_decay, step_decay, g_heads[None], *arrived],
        scratch=[pltpu.VMEM((seqs, DV), f32)],
    )
    near = gathered_tree(mixed, "kv", n_kv)
    far = swapped(near, "kv", n_kv, n_kv // 2)
    (attn_part,) = call(
        dot_kernel,
        [((rows, w_out.shape[1]), bf16)],
        [],
        [near, far, w_out],
    )
    attn_parts = partials_tree(attn_part, "tp", n_tp)
    residual, *blocks = call(
        functools.partial(mix_kernel, n_kv, len(attn_parts), seqs),
        [((rows, columns), bf16)] + [((seqs, 2 * units + LANES), bf16)] * n_kv,
        [place],
        [tokens, g_ffn[None], w_gate, w_up, *attn_parts],
    )
    arrived = [blocks[0]] + [swapped(blocks[r], "kv", n_kv, r) for r in range(1, n_kv)]
    (hidden,) = call(hidden_kernel, [((seqs, units), bf16)], [], arrived)
    (down_part,) = call(
        dot_kernel,
        [((rows, w_down.shape[1]), bf16)],
        [],
        [*partials_direct(hidden, "kv", n_kv), w_down],
    )
    (updated,) = call(
        functools.partial(finish_kernel, n_kv, seqs),
        [((rows, columns), bf16)],
        [place],
        [residual, *partials_tree(down_part, "tp", n_tp)],
    )
    return updated


def solution(mesh):
    sizes = (mesh.shape["kv"], mesh.shape["tp"])
    return jax.shard_map(
        functools.partial(body, sizes),
        mesh=mesh,
        in_specs=(
            P("grp", "kv"),
            P(("grp", "kv")),
            P(("grp", "kv"), "tp", None, None),
            P(("grp", "kv"), "tp", None, None),
            P(("grp", "kv"), "tp", None, None),
            P(("grp", "kv"), "tp", None, None),
            P(("grp", "kv"), "tp"),
            P("kv"),
            P("kv", "tp"),
            P("kv", "tp"),
            P("kv", "tp"),
            P("kv", "tp"),
            P("kv", "tp"),
            P("tp"),
            P("tp", "kv"),
            P("kv"),
            P("kv", "tp"),
            P("kv", "tp"),
            P("tp", "kv"),
        ),
        out_specs=P("grp", "kv"),
        check_vma=False,
    )
```
